32 devices in a mesh: rep: 2 (over x), fs: 8 (over z, y), tp: 2 (over core).
Axes of the slice: x: 2, y: 2, z: 4, core: 2. Of those that a mesh axis runs over, the one named last changes fastest.
Arguments:
- tokens: bfloat16 [12288, 2048], P(('rep', 'fs', 'tp')), may hold values from -6 to 6
- norm_gain: float32 [2048], replicated, may hold values from 0.1 to 1.9
- gate_weight: float32 [2048, 5632], P('fs', 'tp'), may hold values from -0.125 to 0.125
- up_weight: float32 [2048, 5632], P('fs', 'tp'), may hold values from -0.125 to 0.125
- gate_scale: float32 [5632], P('tp'), may hold values from 0.3 to 3
- up_scale: float32 [5632], P('tp'), may hold values from 0.3 to 3
- down_weight: float32 [5632, 2048], P('tp', 'fs'), may hold values from -0.078125 to 0.078125
- down_scale: float32 [2048], replicated, may hold values from 0.3 to 3
Outputs:
- mixed: bfloat16 [12288, 2048], P(('rep', 'fs', 'tp'))
The draws below stay inside these ranges and needn't reach their ends.
All inputs are finite; a program needn't handle non-finite values.
Results may differ from the reference program's by a relative error of at most 0.014.
Values may be sent and summed in bfloat16 or wider, within the bound.
No kernel may reach another device: no remote copies, remote signals or barrier semaphores. Data moves between devices by JAX's collectives and lax.ppermute only.
A program may use at most 128 MiB of HBM per device.

```python
import math
import jax
import jax.numpy as jnp
from jax import lax

D = 2048
FF = 5632
TOKENS = 12288
N_TP = 2


def level_of(own_key, dims, pieces, smallest, largest):
    def one(axis_at, blocks):
        steps = jax.random.uniform(jax.random.fold_in(jax.random.fold_in(own_key, 6), axis_at), (blocks,), jnp.float32, smallest / len(pieces), largest / len(pieces))
        return jnp.repeat(jnp.exp(steps), dims[axis_at] // blocks).reshape((-1,) + (1,) * (len(dims) - axis_at - 1))

    level = one(*pieces[0])
    for cut in pieces[1:]:
        level = level * one(*cut)
    return level


def gaussian(key, extent, scale, bound, cuts=(), held_as=jnp.bfloat16):
    drawn = scale * jax.random.normal(key, extent, jnp.float32)
    if cuts:
        drawn = drawn * level_of(key, extent, cuts, -0.22, 0.18)
    return jnp.clip(drawn, -bound, bound).astype(held_as)


def setup_inputs(seed: int = 0) -> dict:
    splits = jax.random.split(jax.random.key(seed), 9)
    tokens = gaussian(splits[0], (TOKENS, D), 1.0, 6.0, ((0, 32),))
    norm_gain = jnp.clip(1.0 + 0.18 * jax.random.normal(splits[1], (D,), jnp.float32), 0.1, 1.9)
    gate_weight = gaussian(splits[2], (D, FF), D ** -0.5, 0.125, ((0, 8), (1, 2)), jnp.float32)
    up_weight = gaussian(splits[3], (D, FF), D ** -0.5, 0.125, ((0, 8), (1, 2)), jnp.float32)
    gate_scale = jnp.clip(jnp.exp(math.log(3.0) - 2.3025851 * jax.random.uniform(splits[4], (FF,), jnp.float32) ** level_of(splits[4], (FF,), ((0, 2),), -0.2, 0.2)), 0.3, 3.0)
    up_scale = jnp.clip(jnp.exp(math.log(3.0) - 2.3025851 * jax.random.uniform(splits[5], (FF,), jnp.float32) ** level_of(splits[5], (FF,), ((0, 2),), -0.2, 0.2)), 0.3, 3.0)
    down_weight = gaussian(splits[6], (FF, D), FF ** -0.5, 0.078125, ((0, 2), (1, 8)), jnp.float32)
    down_scale = jnp.clip(jnp.exp(jax.random.uniform(splits[7], (D,), jnp.float32, math.log(0.3), math.log(3.0))), 0.3, 3.0)
    return {"tokens": tokens, "norm_gain": norm_gain, "gate_weight": gate_weight, "up_weight": up_weight, "gate_scale": gate_scale, "up_scale": up_scale, "down_weight": down_weight, "down_scale": down_scale}


def reference(tokens, norm_gain, gate_weight, up_weight, gate_scale, up_scale, down_weight, down_scale):
    values = tokens.astype(jnp.float32)
    normed = (values * lax.rsqrt(lax.optimization_barrier(jnp.mean(values * values, axis=-1, keepdims=True)) + 1e-06) * norm_gain).astype(jnp.bfloat16)
    block_width = FF // N_TP
    gate_blocks = gate_weight.astype(jnp.bfloat16).reshape(D, N_TP, block_width).transpose(1, 0, 2)
    up_blocks = up_weight.astype(jnp.bfloat16).reshape(D, N_TP, block_width).transpose(1, 0, 2)
    down_blocks = down_weight.astype(jnp.bfloat16).reshape(N_TP, block_width, D)
    gate_scales = gate_scale.reshape(N_TP, block_width)
    up_scales = up_scale.reshape(N_TP, block_width)

    def one_block(running, blocks):
        gate_piece, up_piece, gate_factor, up_factor, down_piece = blocks
        gate_value = jnp.dot(normed, gate_piece, preferred_element_type=jnp.float32) * gate_factor
        up_value = jnp.dot(normed, up_piece, preferred_element_type=jnp.float32) * up_factor
        hidden = (jax.nn.silu(gate_value) * up_value).astype(jnp.bfloat16)
        partial_value = jnp.dot(hidden, down_piece, preferred_element_type=jnp.float32).astype(jnp.bfloat16)
        return (running + partial_value.astype(jnp.float32), None)
    summed, unused = lax.scan(one_block, jnp.zeros((tokens.shape[0], D), jnp.float32), (gate_blocks, up_blocks, gate_scales, up_scales, down_blocks))
    return (summed * down_scale).astype(jnp.bfloat16)
```

```python
import functools

import jax
import jax.numpy as jnp
from jax import lax
from jax.experimental import pallas as pl
from jax.experimental.pallas import tpu as pltpu
from jax.sharding import Mesh
from jax.sharding import PartitionSpec as P

BF16 = jnp.bfloat16
F32 = jnp.float32
LANES = 128
EPS = 1e-06


def general_plan(
    tokens, norm_gain, gate_weight, up_weight, gate_scale, up_scale, down_weight, down_scale
):
    values = tokens.astype(F32)
    own_normed = (
        values * lax.rsqrt(jnp.mean(values * values, axis=-1, keepdims=True) + EPS) * norm_gain
    ).astype(BF16)
    normed = lax.all_gather(own_normed, "tp", axis=0, tiled=True)
    gate_whole = lax.all_gather(gate_weight.astype(BF16), "fs", axis=0, tiled=True)
    up_whole = lax.all_gather(up_weight.astype(BF16), "fs", axis=0, tiled=True)
    gate_value = jnp.dot(normed, gate_whole, preferred_element_type=F32)
    up_value = jnp.dot(normed, up_whole, preferred_element_type=F32)
    hidden = (jax.nn.silu(gate_value * gate_scale) * (up_value * up_scale)).astype(BF16)
    down_whole = lax.all_gather(down_weight.astype(BF16), "fs", axis=1, tiled=True)
    partial_value = jnp.dot(hidden, down_whole, preferred_element_type=F32).astype(BF16)
    summed = lax.psum_scatter(partial_value, "tp", scatter_dimension=0, tiled=True).astype(F32)
    return (summed * down_scale).astype(BF16)


def pick(index, table):
    value = jnp.int32(table[0])
    for at, entry in enumerate(table[1:], 1):
        value = jnp.where(index == at, jnp.int32(entry), value)
    return value


def ring_order(count):
    return list(range(0, count, 2)) + list(range(1, count, 2))[::-1]


def ring_source(count, step):
    ring = ring_order(count)
    return [ring[(ring.index(z) - step) % count] for z in range(count)]


VM = pl.BlockSpec(memory_space=pltpu.VMEM)
ANY = pl.BlockSpec(memory_space=pl.ANY)


def call(kernel, outs, ins, *, name, flops=0, nbytes=0, **kw):
    kw.setdefault("in_specs", [VM] * len(ins))
    kw.setdefault("out_specs", [VM] * len(outs))
    return pl.pallas_call(
        kernel,
        out_shape=[jax.ShapeDtypeStruct(s, d) for s, d in outs],
        name=name,
        cost_estimate=pl.CostEstimate(
            flops=int(flops), bytes_accessed=int(nbytes), transcendentals=0
        ),
        **kw,
    )(*ins)


def norm_kernel(nz, ny, blk, lo, t_ref, g_ref, lo_ref, hi_ref):
    rows, width = t_ref.shape
    for at in range(0, rows, lo):
        v = t_ref[at : at + lo, :].astype(F32)
        v = v * lax.rsqrt(jnp.mean(v * v, axis=-1, keepdims=True) + EPS) * g_ref[...]
        v = v.astype(BF16)
        for y in range(ny):
            for z in range(nz):
                src, dst = (z * ny + y) * blk, (y * nz + z) * blk
                piece = v[:, src : src + blk]
                if at == 0:
                    lo_ref[:, dst : dst + blk] = piece
                else:
                    hi_ref[at - lo : at, dst : dst + blk] = piece


def prep_kernel(full, cut, g_ref, u_ref, gs_ref, us_ref, a0, b0, a1, b1, sc_ref):
    x, y = lax.axis_index("x"), lax.axis_index("y")
    rest = 4 * full

    def mixed(gr, ur, q):
        at = pl.multiple_of(rest + (q // 2) * LANES, LANES)
        odd = (q % 2) == 1
        g, u = gr[:, pl.ds(at, LANES)], ur[:, pl.ds(at, LANES)]
        half = LANES // 2
        g = jnp.where(odd, pltpu.roll(g, half, 1), g)
        u = jnp.where(odd, u, pltpu.roll(u, half, 1))
        lane = lax.broadcasted_iota(jnp.int32, g.shape, 1)
        return jnp.where(lane < half, g, u)

    for q, a, b in ((2 * x + y, a0, b0), (2 * x + 1 - y, a1, b1)):
        at = pl.multiple_of(q * full, LANES)
        c = cut - full
        a[:, :full] = g_ref[:, pl.ds(at, full)].astype(BF16)
        a[:, full:] = u_ref[:, pl.ds(at, c)].astype(BF16)
        b[:, : full - c] = u_ref[:, pl.ds(pl.multiple_of(at + c, LANES), full - c)].astype(BF16)
        b[:, full - c :] = mixed(g_ref, u_ref, q).astype(BF16)
    q = 2 * x + y
    at = pl.multiple_of(q * full, LANES)
    sc_ref[:, :full] = gs_ref[:, pl.ds(at, full)]
    sc_ref[:, full : 2 * full] = us_ref[:, pl.ds(at, full)]
    sc_ref[:, 2 * full :] = mixed(gs_ref, us_ref, q)


def down_prep_kernel(full, d_ref, own, other):
    x, y = lax.axis_index("x"), lax.axis_index("y")
    half = LANES // 2
    for q, out in ((2 * x + y, own), (2 * x + 1 - y, other)):
        out[:full, :] = d_ref[pl.ds(pl.multiple_of(q * full, 64), full), :].astype(BF16)
        out[full:, :] = d_ref[pl.ds(pl.multiple_of(4 * full + q * half, 64), half), :].astype(BF16)


def gate_up_kernel(nz, blk, full, cut, other, last, *refs):
    refs = list(refs)
    take = lambda n: [refs.pop(0) for _ in range(n)]
    xa, xb = take(2)
    ahead, back = take(nz), take(nz)
    if last:
        scale, acc = take(2)
    (out,) = take(1)
    xs, w, xsem, wsem = take(4)
    y, z = lax.axis_index("y"), lax.axis_index("z")
    i = pl.program_id(0)
    side = 1 - y if other else y
    depth = nz * blk
    nslot = xa.shape[0]

    @pl.when(i == 0)
    def _():
        copies = []
        for s in range(nz):
            f = pl.multiple_of(pick(z, ring_source(nz, s)) * blk, blk)
            b = pl.multiple_of(pick(z, ring_source(nz, -s)) * blk, blk)
            copies.append(
                pltpu.make_async_copy(ahead[s], w.at[pl.ds(f, blk), pl.ds(0, cut)], wsem.at[2 * s])
            )
            copies.append(
                pltpu.make_async_copy(
                    back[s],
                    w.at[pl.ds(b, blk), pl.ds(cut, w.shape[1] - cut)],
                    wsem.at[2 * s + 1],
                )
            )
        for c in copies:
            c.start()
        at = pl.multiple_of(side * depth, depth)
        for k in range(2 * nslot):
            src = xa if k < nslot else xb
            pltpu.make_async_copy(
                src.at[k % nslot, :, pl.ds(at, depth)], xs.at[k], xsem.at[k]
            ).start()
        for c in copies:
            c.wait()

    pltpu.make_async_copy(xa.at[0, :, pl.ds(0, depth)], xs.at[i], xsem.at[i]).wait()
    value = jnp.dot(xs[i], w[...], preferred_element_type=F32)
    if not last:
        out[...] = value
        return
    value = (value + acc[...]) * scale[...]
    g, u, m = value[:, :full], value[:, full : 2 * full], value[:, 2 * full :]
    out[:, :full] = (g / (1 + jnp.exp(-g)) * u).astype(BF16)
    h = m / (1 + jnp.exp(-m)) * pltpu.roll(m, LANES // 2, 1)
    lane = lax.broadcasted_iota(jnp.int32, h.shape, 1)
    out[:, full:] = jnp.where(lane < LANES // 2, h, 0.0).astype(BF16)


def down_kernel(h_ref, a_ref, b_ref, send, keep, w):
    i = pl.program_id(0)
    k, blk = a_ref.shape
    half = keep.shape[0] and pl.num_programs(0) // 2

    @pl.when(i == 0)
    def _():
        w[:k, :blk] = a_ref[...]
        w[:k, blk:] = b_ref[...]
        w[k:, :] = jnp.zeros((w.shape[0] - k, w.shape[1]), BF16)

    value = jnp.dot(h_ref[...], w[...], preferred_element_type=F32).astype(BF16)

    @pl.when(i < half)
    def _():
        send[0] = value

    @pl.when(i >= half)
    def _():
        keep[0] = value


def first_add_kernel(keep, got, ax_keep, ax_send, ay_keep, ay_send):
    blk = ax_keep.shape[2]
    for slot, ax, ay in (
        (0, (ax_keep, 0), (ay_keep, 0)),
        (1, (ax_keep, 1), (ay_send, 0)),
        (2, (ax_send, 0), (ay_keep, 1)),
        (3, (ax_send, 1), (ay_send, 1)),
    ):
        value = (keep[slot].astype(F32) + got[slot].astype(F32)).astype(BF16)
        ax[0][ax[1]] = value[:, :blk]
        ay[0][ay[1]] = value[:, blk:]


def second_add_kernel(ax_keep, ax_got, ay_keep, ay_got, ax, ay):
    ax[...] = (ax_keep[0].astype(F32) + ax_got[0].astype(F32)).astype(BF16)
    ay[...] = (ay_keep[0].astype(F32) + ay_got[0].astype(F32)).astype(BF16)


def final_kernel(nz, blk, *refs):
    ins, scale, out = refs[:-2], refs[-2], refs[-1]
    z = lax.axis_index("z")
    for s in range(nz):
        for j in range(2):
            a, b, c = ins[6 * s + 3 * j : 6 * s + 3 * j + 3]
            source = pick(z, ring_source(nz, s if j == 0 else -s))
            at = pl.ds(pl.multiple_of((2 * source + j) * blk, blk), blk)
            value = a[0].astype(F32) + b[0].astype(F32) + c[...].astype(F32)
            out[:, at] = (value * scale[:, at]).astype(BF16)


def pair_plan(
    nz, tokens, norm_gain, gate_weight, up_weight, gate_scale, up_scale, down_weight, down_scale
):
    rows, width = tokens.shape
    blk, ffl = gate_weight.shape
    full = ffl // (4 * LANES) * LANES
    quarter = ffl // 4
    cut = -(-2 * quarter // (2 * LANES)) * LANES
    hid = full + LANES
    lo = rows // 3
    ring = ring_order(nz)
    ahead = [(ring[p], ring[(p + 1) % nz]) for p in range(nz)]
    back = [(b, a) for a, b in ahead]
    swap = [(0, 1), (1, 0)]
    over = lambda axis, v: lax.ppermute(v, axis, swap)
    y = lax.axis_index("y")

    n_lo, n_hi = call(
        functools.partial(norm_kernel, nz, 2, blk, lo),
        [((lo, width), BF16), ((rows - lo, width), BF16)],
        [tokens, norm_gain.reshape(1, -1)],
        name="norm",
        flops=rows * width * 8,
        nbytes=rows * width * 4,
    )
    a_own, b_own, a_nbr, b_nbr, scale = call(
        functools.partial(prep_kernel, full, cut),
        [
            ((blk, cut), BF16),
            ((blk, 2 * quarter - cut), BF16),
            ((blk, cut), BF16),
            ((blk, 2 * quarter - cut), BF16),
            ((1, 2 * quarter), F32),
        ],
        [gate_weight, up_weight, gate_scale.reshape(1, -1), up_scale.reshape(1, -1)],
        name="prep",
        flops=blk * ffl * 2,
        nbytes=blk * ffl * 12,
    )
    d_own, d_nbr = call(
        functools.partial(down_prep_kernel, full),
        [((quarter, blk), BF16), ((quarter, blk), BF16)],
        [down_weight],
        name="down_prep",
        flops=blk * ffl,
        nbytes=blk * ffl * 6,
    )
    a_far, b_far = over("y", a_nbr), over("y", b_nbr)
    lo_x, lo_y = over("x", n_lo), over("y", n_lo)
    hi_x, hi_y = over("x", n_hi), over("y", n_hi)
    lo_xy, hi_xy = over("y", lo_x), over("x", hi_y)
    d_far = over("y", d_nbr)

    def around(first, hops):
        held = [first]
        for _ in range(nz - 1):
            held.append(lax.ppermute(held[-1], "z", hops))
        return held

    a0, b0 = around(a_own, ahead), around(b_own, back)
    a1, b1 = around(a_far, ahead), around(b_far, back)
    even = jnp.where(y == 0, d_own, d_far)
    odd = jnp.where(y == 0, d_far, d_own)
    d0, d1 = around(even, ahead), around(odd, back)

    xa = jnp.concatenate([n_lo, n_hi, lo_y, hi_y, lo_x, hi_x, lo_xy, hi_xy], axis=0)
    xa = xa.reshape(4, rows, width)
    xb = over("c", xa)

    depth = nz * blk

    def gate_up(a, b, other, extra):
        last = bool(extra)
        wide = hid if last else 2 * quarter
        tile = lambda n: pl.BlockSpec((rows, n), lambda i: (i, 0))
        specs = [ANY] * (2 + 2 * nz)
        if last:
            specs += [VM, tile(2 * quarter)]
        return call(
            functools.partial(gate_up_kernel, nz, blk, full, cut, other, last),
            [((8 * rows, wide), BF16 if last else F32)],
            [xa, xb, *a, *b, *extra],
            name="gate_up_last" if last else "gate_up_first",
            in_specs=specs,
            out_specs=[tile(wide)],
            grid=(8,),
            scratch_shapes=[
                pltpu.VMEM((8, rows, depth), BF16),
                pltpu.VMEM((depth, 2 * quarter), BF16),
                pltpu.SemaphoreType.DMA((8,)),
                pltpu.SemaphoreType.DMA((2 * nz,)),
            ],
            flops=8 * rows * depth * 4 * quarter,
            nbytes=8 * rows * (2 * depth + 8 * quarter),
        )[0]

    acc = gate_up(a0, b0, False, ())
    hidden = gate_up(a1, b1, True, (scale, acc))

    parts = []
    for s in range(nz):
        send, keep = call(
            down_kernel,
            [((4, rows, 2 * blk), BF16), ((4, rows, 2 * blk), BF16)],
            [hidden, d0[s], d1[s]],
            name="down",
            grid=(8,),
            in_specs=[
                pl.BlockSpec((rows, hid), lambda i: ((i + 4) % 8, 0)),
                VM,
                VM,
            ],
            out_specs=[
                pl.BlockSpec((1, rows, 2 * blk), lambda i: (jnp.minimum(i, 3), 0, 0)),
                pl.BlockSpec((1, rows, 2 * blk), lambda i: (jnp.maximum(i - 4, 0), 0, 0)),
            ],
            scratch_shapes=[pltpu.VMEM((hid, 2 * blk), BF16)],
            flops=8 * rows * hid * 4 * blk,
            nbytes=8 * rows * (hid + 2 * blk) * 2,
        )
        got = over("c", send)
        pair = ((2, rows, blk), BF16)
        ax_keep, ax_send, ay_keep, ay_send = call(
            first_add_kernel,
            [pair] * 4,
            [keep, got],
            name="first_add",
            flops=4 * rows * blk * 2,
            nbytes=4 * rows * blk * 12,
        )
        ax_got, ay_got = over("x", ax_send), over("y", ay_send)
        second = pl.BlockSpec((1, rows, blk), lambda i: (1, 0, 0))
        whole = pl.BlockSpec((rows, blk), lambda i: (0, 0))
        ax_next, ay_next = call(
            second_add_kernel,
            [((rows, blk), BF16)] * 2,
            [ax_keep, ax_got, ay_keep, ay_got],
            name="second_add",
            grid=(1,),
            in_specs=[second] * 4,
            out_specs=[whole] * 2,
            flops=4 * rows * blk,
            nbytes=2 * rows * blk * 6,
        )
        parts += [ax_keep, ax_got, over("y", ax_next), ay_keep, ay_got, over("x", ay_next)]

    third = pl.BlockSpec((1, lo, blk), lambda i: (0, i, 0))
    flat = pl.BlockSpec((lo, blk), lambda i: (i, 0))
    return call(
        functools.partial(final_kernel, nz, blk),
        [((rows, width), BF16)],
        [*parts, down_scale.reshape(1, -1)],
        name="final",
        grid=(rows // lo,),
        in_specs=[third, third, flat] * (2 * nz) + [VM],
        out_specs=[pl.BlockSpec((lo, width), lambda i: (i, 0))],
        flops=rows * width * 4,
        nbytes=rows * width * 8,
    )[0]


def solution(mesh):
    reps, shards, cores = (mesh.shape[a] for a in ("rep", "fs", "tp"))

    def run(*args):
        tokens, gate = args[0], args[2]
        rows = tokens.shape[0] // (reps * shards * cores)
        ffl, blk = gate.shape[1] // cores, gate.shape[0] // shards
        paired = (
            reps == 2
            and cores == 2
            and shards % 2 == 0
            and shards > 2
            and ffl % LANES == 0
            and ffl % (4 * LANES) == 2 * LANES
            and blk % LANES == 0
            and rows % 48 == 0
        )
        if paired:
            nz = shards // 2
            grid = Mesh(mesh.devices.reshape(reps, nz, 2, cores), ("x", "z", "y", "c"))
            row, deep, wide = ("x", "z", "y", "c"), ("z", "y"), "c"
            body = functools.partial(pair_plan, nz)
        else:
            grid, body = mesh, general_plan
            row, deep, wide = ("rep", "fs", "tp"), "fs", "tp"
        return jax.shard_map(
            body,
            mesh=grid,
            in_specs=(
                P(row, None),
                P(),
                P(deep, wide),
                P(deep, wide),
                P(wide),
                P(wide),
                P(wide, deep),
                P(),
            ),
            out_specs=P(row, None),
            check_vma=False,
        )(*args)

    return run
```

```python
import functools

import jax
import jax.numpy as jnp
from jax import lax
from jax.experimental import pallas as pl
from jax.experimental.pallas import tpu as pltpu
from jax.sharding import Mesh
from jax.sharding import PartitionSpec as P


BF16 = jnp.bfloat16
F32 = jnp.float32
LANES = 128
EPS = 1e-06


def general_plan(
    tokens, norm_gain, gate_weight, up_weight, gate_scale, up_scale, down_weight, down_scale
):
    values = tokens.astype(F32)
    own_normed = (
        values * lax.rsqrt(jnp.mean(values * values, axis=-1, keepdims=True) + EPS) * norm_gain
    ).astype(BF16)
    normed = lax.all_gather(own_normed, "tp", axis=0, tiled=True)
    gate_whole = lax.all_gather(gate_weight.astype(BF16), "fs", axis=0, tiled=True)
    up_whole = lax.all_gather(up_weight.astype(BF16), "fs", axis=0, tiled=True)
    gate_value = jnp.dot(normed, gate_whole, preferred_element_type=F32)
    up_value = jnp.dot(normed, up_whole, preferred_element_type=F32)
    hidden = (jax.nn.silu(gate_value * gate_scale) * (up_value * up_scale)).astype(BF16)
    down_whole = lax.all_gather(down_weight.astype(BF16), "fs", axis=1, tiled=True)
    partial_value = jnp.dot(hidden, down_whole, preferred_element_type=F32).astype(BF16)
    summed = lax.psum_scatter(partial_value, "tp", scatter_dimension=0, tiled=True).astype(F32)
    return (summed * down_scale).astype(BF16)


def pick(index, table):
    value = jnp.int32(table[0])
    for at, entry in enumerate(table[1:], 1):
        value = jnp.where(index == at, jnp.int32(entry), value)
    return value


def ring_order(count):
    return list(range(0, count, 2)) + list(range(1, count, 2))[::-1]


def ring_source(count, step):
    ring = ring_order(count)
    return [ring[(ring.index(z) - step) % count] for z in range(count)]


VM = pl.BlockSpec(memory_space=pltpu.VMEM)
ANY = pl.BlockSpec(memory_space=pl.ANY)


def call(kernel, outs, ins, *, flops=0, nbytes=0, **kw):
    kw.setdefault("in_specs", [VM] * len(ins))
    kw.setdefault("out_specs", [VM] * len(outs))
    return pl.pallas_call(
        kernel,
        out_shape=[jax.ShapeDtypeStruct(s, d) for s, d in outs],
        cost_estimate=pl.CostEstimate(
            flops=int(flops), bytes_accessed=int(nbytes), transcendentals=0
        ),
        **kw,
    )(*ins)


def norm_kernel(lo, t_ref, g_ref, lo_ref, hi_ref):
    rows = t_ref.shape[0]
    for at in range(0, rows, lo):
        v = t_ref[at : at + lo, :].astype(F32)
        v = v * lax.rsqrt(jnp.mean(v * v, axis=-1, keepdims=True) + EPS) * g_ref[...]
        if at == 0:
            lo_ref[...] = v.astype(BF16)
        else:
            hi_ref[at - lo : at, :] = v.astype(BF16)


def mixed(gr, ur, q, full):
    at = pl.multiple_of(4 * full + (q // 2) * LANES, LANES)
    odd = (q % 2) == 1
    g, u = gr[:, pl.ds(at, LANES)], ur[:, pl.ds(at, LANES)]
    half = LANES // 2
    g = jnp.where(odd, pltpu.roll(g, half, 1), g)
    u = jnp.where(odd, u, pltpu.roll(u, half, 1))
    lane = lax.broadcasted_iota(jnp.int32, g.shape, 1)
    return jnp.where(lane < half, g, u)


def take(gr, ur, q, full, first, one, two):
    second = full - first
    at = pl.multiple_of(q * full, LANES)
    later = pl.multiple_of(q * full + first, LANES)
    kind = one.dtype
    one[:, :first] = gr[:, pl.ds(at, first)].astype(kind)
    one[:, first:] = ur[:, pl.ds(at, first)].astype(kind)
    two[:, :second] = gr[:, pl.ds(later, second)].astype(kind)
    two[:, second : 2 * second] = ur[:, pl.ds(later, second)].astype(kind)
    two[:, 2 * second :] = mixed(gr, ur, q, full).astype(kind)


def prep_kernel(full, first, g_ref, u_ref, own1, own2, far1, far2):
    x, y = lax.axis_index("x"), lax.axis_index("y")
    take(g_ref, u_ref, 2 * x + y, full, first, own1, own2)
    take(g_ref, u_ref, 2 * x + 1 - y, full, first, far1, far2)


def scale_kernel(full, first, g_ref, u_ref, out):
    x, y = lax.axis_index("x"), lax.axis_index("y")
    take(g_ref, u_ref, 2 * x + y, full, first, out.at[:, : 2 * first], out.at[:, 2 * first :])


def down_prep_kernel(full, d_ref, own, other):
    x, y = lax.axis_index("x"), lax.axis_index("y")
    half = LANES // 2
    for q, out in ((2 * x + y, own), (2 * x + 1 - y, other)):
        out[:full, :] = d_ref[pl.ds(pl.multiple_of(q * full, 64), full), :].astype(BF16)
        out[full:, :] = d_ref[pl.ds(pl.multiple_of(4 * full + q * half, 64), half), :].astype(BF16)


def gate_up_kernel(nz, blk, part, x_ref, s_own, s_oth, *refs):
    pieces, (out, w, wsem) = refs[: 4 * nz], refs[4 * nz :]
    y, z = lax.axis_index("y"), lax.axis_index("z")
    n = s_own.shape[1]

    @pl.when(pl.program_id(0) == 0)
    def _():
        copies = []
        for s in range(nz):
            f = 2 * pick(z, ring_source(nz, s)) + y
            b = 2 * pick(z, ring_source(nz, -s)) + 1 - y
            for k, at in enumerate((f, b, f, b)):
                rows = pl.ds(pl.multiple_of(at * blk, blk), blk)
                dst = w.at[rows, pl.ds(n * (k // 2), n)]
                copies.append(pltpu.make_async_copy(pieces[k * nz + s], dst, wsem.at[4 * s + k]))
        for c in copies:
            c.start()
        for c in copies:
            c.wait()

    value = jnp.dot(x_ref[...], w[...], preferred_element_type=F32)
    tails = []
    for at, scale in ((0, s_own), (1, s_oth)):
        v = value[:, at * n : (at + 1) * n] * scale[...]
        g, u = v[:, :part], v[:, part : 2 * part]
        out[:, at * part : (at + 1) * part] = (g / (1 + jnp.exp(-g)) * u).astype(BF16)
        if n > 2 * part:
            m = v[:, 2 * part :]
            tails.append(m / (1 + jnp.exp(-m)) * pltpu.roll(m, LANES // 2, 1))
    if tails:
        h, o = tails
        lane = lax.broadcasted_iota(jnp.int32, h.shape, 1)
        o = pltpu.roll(o, LANES // 2, 1)
        out[:, 2 * part :] = jnp.where(lane < LANES // 2, h, o).astype(BF16)


def down_kernel(cuts, h1, h2, a_own, a_oth, b_own, b_oth, ax_keep, ax_send, ay_keep, ay_send, w):
    i = pl.program_id(0)
    blk = a_own.shape[1]

    @pl.when(i == 0)
    def _():
        at = 0
        for lo, hi in cuts:
            for own, left in ((True, at), (False, at + hi - lo)):
                w[left : left + hi - lo, :blk] = (a_own if own else a_oth)[lo:hi, :]
                w[left : left + hi - lo, blk:] = (b_own if own else b_oth)[lo:hi, :]
            at += 2 * (hi - lo)

    n = h1.shape[1]
    value = jnp.dot(h1[...], w[:n], preferred_element_type=F32) + jnp.dot(
        h2[...], w[n:], preferred_element_type=F32
    )
    value = value.astype(BF16)
    left, right = value[:, :blk], value[:, blk:]

    @pl.when(i < 2)
    def _():
        ax_keep[0] = left

    @pl.when(i >= 2)
    def _():
        ax_send[0] = left

    @pl.when(i % 2 == 0)
    def _():
        ay_keep[0] = right

    @pl.when(i % 2 == 1)
    def _():
        ay_send[0] = right


def second_add_kernel(ax_keep, ax_got, ay_keep, ay_got, ax, ay):
    ax[...] = (ax_keep[0].astype(F32) + ax_got[0].astype(F32)).astype(BF16)
    ay[...] = (ay_keep[0].astype(F32) + ay_got[0].astype(F32)).astype(BF16)


def final_kernel(nz, blk, *refs):
    ins, scale, out = refs[:-2], refs[-2], refs[-1]
    z = lax.axis_index("z")
    for s in range(nz):
        for j in range(2):
            a, b, c = ins[6 * s + 3 * j : 6 * s + 3 * j + 3]
            source = pick(z, ring_source(nz, s if j == 0 else -s))
            at = pl.ds(pl.multiple_of((2 * source + j) * blk, blk), blk)
            value = a[0].astype(F32) + b[0].astype(F32) + c[...].astype(F32)
            out[:, at] = (value * scale[:, at]).astype(BF16)


def after(value, *others):
    return lax.optimization_barrier((value, *others))[0]


def pair_plan(
    nz, tokens, norm_gain, gate_weight, up_weight, gate_scale, up_scale, down_weight, down_scale
):
    rows, width = tokens.shape
    blk, ffl = gate_weight.shape
    full = ffl // (4 * LANES) * LANES
    quarter = ffl // 4
    first = max(LANES, full - LANES)
    second = full - first
    wide1, wide2 = 2 * first, 2 * second + LANES
    lo = rows // 3
    ring = ring_order(nz)
    ahead = [(ring[p], ring[(p + 1) % nz]) for p in range(nz)]
    back = [(b, a) for a, b in ahead]
    swap = [(0, 1), (1, 0)]
    y = lax.axis_index("y")

    def send(v, axis, hops=swap):
        return lax.ppermute(v, axis, hops)

    own1, own2, far1, far2 = call(
        functools.partial(prep_kernel, full, first),
        [((blk, wide1), BF16), ((blk, wide2), BF16)] * 2,
        [gate_weight, up_weight],
        flops=blk * ffl * 2,
        nbytes=blk * ffl * 12,
    )
    hop = lambda v: send(v, "z", ahead)
    pop = lambda v: send(v, "z", back)
    c1, c2 = [own1, hop(own1)], [own2, hop(own2)]
    g1 = [send(far1, "y")]
    n_lo, n_hi = call(
        functools.partial(norm_kernel, lo),
        [((lo, width), BF16), ((rows - lo, width), BF16)],
        [after(tokens, own1), norm_gain.reshape(1, -1)],
        flops=rows * width * 8,
        nbytes=rows * width * 4,
    )
    hi_x, hi_y = send(n_hi, "x"), send(n_hi, "y")
    d_own, d_nbr = call(
        functools.partial(down_prep_kernel, full),
        [((quarter, blk), BF16), ((quarter, blk), BF16)],
        [after(down_weight, n_hi)],
        flops=blk * ffl,
        nbytes=blk * ffl * 6,
    )
    (scale,) = call(
        functools.partial(scale_kernel, full, first),
        [((1, 2 * quarter), F32)],
        [after(gate_scale, d_own).reshape(1, -1), after(up_scale, d_own).reshape(1, -1)],
        flops=ffl,
        nbytes=ffl * 8,
    )
    scale_oth = send(scale, "c")
    clock = d_own

    def event(value):
        nonlocal clock
        clock = after(value, clock)
        return clock

    across = {}

    def twin(name, v):
        across[name] = send(v, "c")

    twin("c10", own1)
    twin("c20", own2)
    c1[1] = event(c1[1])
    c1.append(hop(c1[1]))
    twin("c11", c1[1])
    lo_x = send(after(n_lo, clock), "x")
    g1[0] = event(g1[0])
    g1.append(pop(g1[0]))
    twin("g10", g1[0])
    g2 = [send(after(far2, clock), "y")]
    c2[1] = event(c2[1])
    twin("c21", c2[1])
    lo_y = send(after(n_lo, clock), "y")
    c1[2] = event(c1[2])
    c1.append(hop(c1[2]))
    twin("c12", c1[2])
    hi_x = event(hi_x)
    g1[1] = event(g1[1])
    g1.append(pop(g1[1]))
    twin("g11", g1[1])
    hi_y = event(hi_y)
    hi_xy = send(hi_y, "x")
    lo_x = event(lo_x)
    lo_xy = send(lo_x, "y")
    g2[0] = event(g2[0])
    twin("g20", g2[0])
    c1[3] = event(c1[3])
    c2.append(hop(after(c2[1], clock)))
    twin("c13", c1[3])
    g1[2] = event(g1[2])
    g1.append(pop(g1[2]))
    g2.append(pop(after(g2[0], clock)))
    twin("g12", g1[2])
    lo_y = event(lo_y)
    hi_xy = event(hi_xy)
    lo_xy = event(lo_xy)
    xa = jnp.concatenate([n_lo, n_hi, lo_y, hi_y, lo_x, hi_x, lo_xy, hi_xy], axis=0)
    clock = xa
    d_far = send(after(d_nbr, clock), "y")
    c2[2] = event(c2[2])
    c2.append(hop(c2[2]))
    twin("c22", c2[2])
    g1[3] = event(g1[3])
    twin("g13", g1[3])
    g2[1] = event(g2[1])
    g2.append(pop(g2[1]))
    twin("g21", g2[1])

    def gate_up(at, own, far, part, rows_in):
        n = wide1 if at == 1 else wide2
        cols = slice(0, n) if at == 1 else slice(wide1, wide1 + n)
        wide = 2 * part + (LANES if at == 2 else 0)
        twins = [across[f"c{at}{s}"] for s in range(nz)] + [across[f"g{at}{s}"] for s in range(nz)]
        tile = lambda n: pl.BlockSpec((rows, n), lambda i: (i, 0))
        return call(
            functools.partial(gate_up_kernel, nz, blk, part),
            [((4 * rows, wide), BF16)],
            [rows_in, scale[:, cols], scale_oth[:, cols], *own, *far, *twins],
            in_specs=[tile(width), VM, VM] + [ANY] * (4 * nz),
            out_specs=[tile(wide)],
            grid=(4,),
            scratch_shapes=[
                pltpu.VMEM((width, 2 * n), BF16),
                pltpu.SemaphoreType.DMA((4 * nz,)),
            ],
            flops=4 * rows * width * n * 4,
            nbytes=4 * rows * (width + wide) * 2 + width * n * 4,
        )[0]

    h1 = gate_up(1, c1, g1, first, after(xa, clock))
    clock = h1
    c2[3] = event(c2[3])
    twin("c23", c2[3])
    g2[2] = event(g2[2])
    g2.append(pop(g2[2]))
    twin("g22", g2[2])
    d_far = event(d_far)
    even = [jnp.where(y == 0, d_own, d_far)]
    odd = [jnp.where(y == 0, d_far, d_own)]
    even.append(hop(even[0]))
    odd.append(pop(odd[0]))
    twin("e0", even[0])
    twin("o0", odd[0])
    g2[3] = event(g2[3])
    twin("g23", g2[3])
    h2 = gate_up(2, c2, g2, second, after(xa, clock))
    clock = h2

    cuts = ((0, first), (first, full), (full, quarter))

    def down(s):
        tile = lambda n: pl.BlockSpec((rows, n), lambda i: (i, 0))
        slot = lambda f: pl.BlockSpec((1, rows, blk), lambda i: (f(i), 0, 0))
        return call(
            functools.partial(down_kernel, cuts),
            [((2, rows, blk), BF16)] * 4,
            [after(h1, clock), h2, even[s], across[f"e{s}"], odd[s], across[f"o{s}"]],
            in_specs=[tile(h1.shape[1]), tile(h2.shape[1])] + [VM] * 4,
            out_specs=[
                slot(lambda i: jnp.minimum(i, 1)),
                slot(lambda i: jnp.maximum(i - 2, 0)),
                slot(lambda i: i // 2),
                slot(lambda i: i // 2),
            ],
            grid=(4,),
            scratch_shapes=[pltpu.VMEM((2 * quarter, 2 * blk), BF16)],
            flops=4 * rows * quarter * 8 * blk,
            nbytes=4 * rows * (2 * quarter + 2 * blk) * 2,
        )

    def second_add(*ins):
        one = pl.BlockSpec((1, rows, blk), lambda i: (1, 0, 0))
        whole = pl.BlockSpec((rows, blk), lambda i: (0, 0))
        return call(
            second_add_kernel,
            [((rows, blk), BF16)] * 2,
            list(ins),
            grid=(1,),
            in_specs=[one] * 4,
            out_specs=[whole] * 2,
            flops=4 * rows * blk,
            nbytes=2 * rows * blk * 6,
        )

    parts = []
    flying = None

    def land():
        nonlocal clock
        _, ax_keep, ax_got, ay_keep, ay_got = flying
        ax_got, ay_got = event(ax_got), event(ay_got)
        ax_next, ay_next = second_add(ax_keep, ax_got, ay_keep, ay_got)
        clock = ax_next
        parts.extend([ax_keep, ax_got, send(ax_next, "y")])
        parts.extend([ay_keep, ay_got, send(ay_next, "x")])

    for s in range(nz):
        ax_keep, ax_send, ay_keep, ay_send = down(s)
        clock = ax_keep
        now = (s, ax_keep, send(ax_send, "x"), ay_keep, send(ay_send, "y"))
        if s + 1 < nz:
            even[s + 1] = event(even[s + 1])
            odd[s + 1] = event(odd[s + 1])
            if s + 2 < nz:
                even.append(hop(even[s + 1]))
                odd.append(pop(odd[s + 1]))
            twin(f"e{s + 1}", even[s + 1])
            twin(f"o{s + 1}", odd[s + 1])
        if flying:
            land()
        flying = now
    land()

    third = pl.BlockSpec((1, lo, blk), lambda i: (0, i, 0))
    flat = pl.BlockSpec((lo, blk), lambda i: (i, 0))
    return call(
        functools.partial(final_kernel, nz, blk),
        [((rows, width), BF16)],
        [*parts, down_scale.reshape(1, -1)],
        grid=(rows // lo,),
        in_specs=[third, third, flat] * (2 * nz) + [VM],
        out_specs=[pl.BlockSpec((lo, width), lambda i: (i, 0))],
        flops=rows * width * 4,
        nbytes=rows * width * 8,
    )[0]


def solution(mesh):
    reps, shards, cores = (mesh.shape[a] for a in ("rep", "fs", "tp"))

    def run(*args):
        tokens, gate = args[0], args[2]
        rows = tokens.shape[0] // (reps * shards * cores)
        ffl, blk = gate.shape[1] // cores, gate.shape[0] // shards
        paired = (
            reps == 2
            and cores == 2
            and shards % 2 == 0
            and shards > 2
            and ffl % LANES == 0
            and ffl % (4 * LANES) == 2 * LANES
            and blk % LANES == 0
            and rows % 48 == 0
        )
        if paired:
            nz = shards // 2
            grid = Mesh(mesh.devices.reshape(reps, nz, 2, cores), ("x", "z", "y", "c"))
            row, deep, wide = ("x", "z", "y", "c"), ("z", "y"), "c"
            plan = functools.partial(pair_plan, nz)

            def body(*args):
                return plan(*args)

        else:
            grid, body = mesh, general_plan
            row, deep, wide = ("rep", "fs", "tp"), "fs", "tp"
        step = jax.shard_map(
            body,
            mesh=grid,
            in_specs=(
                P(row, None),
                P(),
                P(deep, wide),
                P(deep, wide),
                P(wide),
                P(wide),
                P(wide, deep),
                P(),
            ),
            out_specs=P(row, None),
            check_vma=False,
        )
        return step(*args)

    return run
```

```python
import functools

import jax
import jax.numpy as jnp
from jax import lax
from jax.experimental import pallas as pl
from jax.experimental.pallas import tpu as pltpu
from jax.sharding import Mesh
from jax.sharding import PartitionSpec as P


BF16 = jnp.bfloat16
F32 = jnp.float32
LANES = 128
EPS = 1e-06


def general_plan(
    tokens, norm_gain, gate_weight, up_weight, gate_scale, up_scale, down_weight, down_scale
):
    values = tokens.astype(F32)
    own_normed = (
        values * lax.rsqrt(jnp.mean(values * values, axis=-1, keepdims=True) + EPS) * norm_gain
    ).astype(BF16)
    normed = lax.all_gather(own_normed, "tp", axis=0, tiled=True)
    gate_whole = lax.all_gather(gate_weight.astype(BF16), "fs", axis=0, tiled=True)
    up_whole = lax.all_gather(up_weight.astype(BF16), "fs", axis=0, tiled=True)
    gate_value = jnp.dot(normed, gate_whole, preferred_element_type=F32)
    up_value = jnp.dot(normed, up_whole, preferred_element_type=F32)
    hidden = (jax.nn.silu(gate_value * gate_scale) * (up_value * up_scale)).astype(BF16)
    down_whole = lax.all_gather(down_weight.astype(BF16), "fs", axis=1, tiled=True)
    partial_value = jnp.dot(hidden, down_whole, preferred_element_type=F32).astype(BF16)
    summed = lax.psum_scatter(partial_value, "tp", scatter_dimension=0, tiled=True).astype(F32)
    return (summed * down_scale).astype(BF16)


def pick(index, table):
    value = jnp.int32(table[0])
    for at, entry in enumerate(table[1:], 1):
        value = jnp.where(index == at, jnp.int32(entry), value)
    return value


def ring_order(count):
    return list(range(0, count, 2)) + list(range(1, count, 2))[::-1]


def ring_source(count, step):
    ring = ring_order(count)
    return [ring[(ring.index(z) - step) % count] for z in range(count)]


VM = pl.BlockSpec(memory_space=pltpu.VMEM)
ANY = pl.BlockSpec(memory_space=pltpu.HBM)


def call(kernel, outs, ins, *, flops=0, nbytes=0, **kw):
    kw.setdefault("in_specs", [VM] * len(ins))
    kw.setdefault("out_specs", [VM] * len(outs))
    return pl.pallas_call(
        kernel,
        out_shape=[jax.ShapeDtypeStruct(s, d) for s, d in outs],
        cost_estimate=pl.CostEstimate(
            flops=int(flops), bytes_accessed=int(nbytes), transcendentals=0
        ),
        **kw,
    )(*ins)


def norm_kernel(lo, t_ref, g_ref, lo_ref, hi_ref):
    rows = t_ref.shape[0]
    for at in range(0, rows, lo):
        v = t_ref[at : at + lo, :].astype(F32)
        v = v * lax.rsqrt(jnp.mean(v * v, axis=-1, keepdims=True) + EPS) * g_ref[...]
        if at == 0:
            lo_ref[...] = v.astype(BF16)
        else:
            hi_ref[at - lo : at, :] = v.astype(BF16)


def prep_kernel(full, first, which, g_ref, u_ref, *refs):
    outs, (held, sems) = refs[:-2], refs[-2:]
    x, y = lax.axis_index("x"), lax.axis_index("y")
    half = LANES // 2
    second = full - first
    copies, at = [], 0

    def fetch(src, start, n):
        nonlocal at
        dst = held.at[:, pl.ds(at, n)]
        copy = pltpu.make_async_copy(src.at[:, pl.ds(start, n)], dst, sems.at[len(copies)])
        copy.start()
        copies.append((copy, at, n))
        at += n

    for far, late in which:
        q = 2 * x + (1 - y if far else y)
        start = pl.multiple_of(q * full + (first if late else 0), LANES)
        for src in (g_ref, u_ref):
            fetch(src, start, second if late else first)
        if late:
            start = pl.multiple_of(4 * full + (q // 2) * LANES, LANES)
            for src in (g_ref, u_ref):
                fetch(src, start, LANES)
    rest = list(copies)

    def arrived():
        copy, at, n = rest.pop(0)
        copy.wait()
        return held[:, at : at + n]

    for out, (far, late) in zip(outs, which):
        odd = ((1 - y if far else y) % 2) == 1
        n = second if late else first
        out[:, :n] = arrived().astype(BF16)
        out[:, n : 2 * n] = arrived().astype(BF16)
        if late:
            g, u = arrived(), arrived()
            g = jnp.where(odd, pltpu.roll(g, half, 1), g)
            u = jnp.where(odd, u, pltpu.roll(u, half, 1))
            lane = lax.broadcasted_iota(jnp.int32, g.shape, 1)
            out[:, 2 * n :] = jnp.where(lane < half, g, u).astype(BF16)


def scale_kernel(full, first, g_ref, u_ref, out):
    x, y = lax.axis_index("x"), lax.axis_index("y")
    q, half = 2 * x + y, LANES // 2
    at = 0
    for lo, hi in ((0, first), (first, full)):
        for ref in (g_ref, u_ref):
            for k in range(lo // LANES, hi // LANES):
                out[:, at : at + LANES] = ref[pl.ds(q * (full // LANES) + k, 1), :]
                at += LANES
    row = pl.ds(4 * full // LANES + q // 2, 1)
    odd = (q % 2) == 1
    g, u = g_ref[row, :], u_ref[row, :]
    g = jnp.where(odd, pltpu.roll(g, half, 1), g)
    u = jnp.where(odd, u, pltpu.roll(u, half, 1))
    out[:, at:] = jnp.where(lax.broadcasted_iota(jnp.int32, g.shape, 1) < half, g, u)


def down_prep_kernel(full, d_ref, own, other):
    x, y = lax.axis_index("x"), lax.axis_index("y")
    half = LANES // 2
    for q, out in ((2 * x + y, own), (2 * x + 1 - y, other)):
        out[:full, :] = d_ref[pl.ds(pl.multiple_of(q * full, 64), full), :].astype(BF16)
        out[full:, :] = d_ref[pl.ds(pl.multiple_of(4 * full + q * half, 64), half), :].astype(BF16)


def gate_up_kernel(nz, blk, part, cols, slots, s_own, s_oth, *refs):
    tokens, refs = refs[: 2 * slots], refs[2 * slots :]
    pieces, (out, xs, w, xsem, wsem) = refs[: 4 * nz], refs[4 * nz :]
    y, z = lax.axis_index("y"), lax.axis_index("z")
    n = pieces[0].shape[1]
    lo = tokens[0].shape[0]
    i = pl.program_id(0)

    @pl.when(i == 0)
    def _():
        copies = []
        for s in range(nz):
            f = 2 * pick(z, ring_source(nz, s)) + y
            b = 2 * pick(z, ring_source(nz, -s)) + 1 - y
            for k, at in enumerate((f, b, f, b)):
                rows = pl.ds(pl.multiple_of(at * blk, blk), blk)
                dst = w.at[rows, pl.ds(n * (k // 2), n)]
                copies.append(pltpu.make_async_copy(pieces[k * nz + s], dst, wsem.at[4 * s + k]))
        for c in copies:
            c.start()
        for k, ref in enumerate(tokens):
            rows = pl.ds(lo, ref.shape[0]) if k % 2 else pl.ds(0, lo)
            pltpu.make_async_copy(ref, xs.at[k // 2, rows], xsem.at[k]).start()
        for c in copies:
            c.wait()

    pltpu.make_async_copy(tokens[0], xs.at[i, pl.ds(0, lo)], xsem.at[2 * i]).wait()
    rest = xs.shape[1] - lo
    pltpu.make_async_copy(tokens[1], xs.at[i, pl.ds(lo, rest)], xsem.at[2 * i + 1]).wait()
    value = jnp.dot(xs[i], w[...], preferred_element_type=F32)
    tails = []
    for at, scale in ((0, s_own), (1, s_oth)):
        v = value[:, at * n : (at + 1) * n] * scale[:, cols : cols + n]
        g, u = v[:, :part], v[:, part : 2 * part]
        out[:, at * part : (at + 1) * part] = (g / (1 + jnp.exp(-g)) * u).astype(BF16)
        if n > 2 * part:
            m = v[:, 2 * part :]
            tails.append(m / (1 + jnp.exp(-m)) * pltpu.roll(m, LANES // 2, 1))
    if tails:
        h, o = tails
        lane = lax.broadcasted_iota(jnp.int32, h.shape, 1)
        o = pltpu.roll(o, LANES // 2, 1)
        out[:, 2 * part :] = jnp.where(lane < LANES // 2, h, o).astype(BF16)


def down_kernel(cuts, count, h1, h2, *refs):
    pieces, refs = refs[: 4 * count], refs[4 * count :]
    ax_keep, ax_send, ay_keep, ay_send, w, sems = refs
    i = pl.program_id(0)
    blk = pieces[0].shape[1]
    rows = h1.shape[0] // 2

    @pl.when(i == 0)
    def _():
        copies = []
        for k in range(2 * count):
            cols = pl.ds(((k % 2) * count + k // 2) * blk, blk)
            at = 0
            for lo, hi in cuts:
                for piece in pieces[2 * k : 2 * k + 2]:
                    src, dst = piece.at[pl.ds(lo, hi - lo), :], w.at[pl.ds(at, hi - lo), cols]
                    copies.append(pltpu.make_async_copy(src, dst, sems.at[len(copies)]))
                    at += hi - lo
        for copy in copies:
            copy.start()
        for copy in copies:
            copy.wait()

    n = h1.shape[1]
    value = jnp.dot(h1[...], w[:n], preferred_element_type=F32) + jnp.dot(
        h2[...], w[n:], preferred_element_type=F32
    )
    value = value.astype(BF16)
    left, right = value[:, : count * blk], value[:, count * blk :]
    ay_keep[0], ay_send[0] = right[:rows], right[rows:]

    @pl.when(i == 0)
    def _():
        ax_keep[0], ax_keep[1] = left[:rows], left[rows:]

    @pl.when(i == 1)
    def _():
        ax_send[0], ax_send[1] = left[:rows], left[rows:]


def second_add_kernel(ax_keep, ax_got, ay_keep, ay_got, ax, ay):
    ax[...] = (ax_keep[0].astype(F32) + ax_got[0].astype(F32)).astype(BF16)
    ay[...] = (ay_keep[0].astype(F32) + ay_got[0].astype(F32)).astype(BF16)


def final_kernel(nz, blk, groups, aliased, *refs):
    ins, scale, refs = refs[: 6 * len(groups)], refs[6 * len(groups)], refs[6 * len(groups) + 1 :]
    out, held, sems = refs[1:] if aliased else refs
    z = lax.axis_index("z")
    copies = []
    for n, group in enumerate(groups):
        for j in range(2):
            a, b, c = ins[6 * n + 3 * j : 6 * n + 3 * j + 3]
            for k, s in enumerate(group):
                source = pick(z, ring_source(nz, s if j == 0 else -s))
                at = pl.ds(pl.multiple_of((2 * source + j) * blk, blk), blk)
                here = slice(k * blk, (k + 1) * blk)
                value = a[0, :, here].astype(F32) + b[0, :, here].astype(F32)
                value = value + c[:, here].astype(F32)
                slot = len(copies)
                held[slot] = (value * scale[:, at]).astype(BF16)
                copies.append(pltpu.make_async_copy(held.at[slot], out.at[:, at], sems.at[slot]))
                copies[-1].start()
    for copy in copies:
        copy.wait()


def after(value, *others):
    return lax.optimization_barrier((value, *others))[0]


def pair_plan(
    nz, tokens, norm_gain, gate_weight, up_weight, gate_scale, up_scale, down_weight, down_scale
):
    rows, width = tokens.shape
    blk, ffl = gate_weight.shape
    full = ffl // (4 * LANES) * LANES
    quarter = ffl // 4
    first = -(-full // (2 * LANES)) * LANES
    second = full - first
    wide1, wide2 = 2 * first, 2 * second + LANES
    lo = rows // 3
    ring = ring_order(nz)
    ahead = [(ring[p], ring[(p + 1) % nz]) for p in range(nz)]
    back = [(b, a) for a, b in ahead]
    swap = [(0, 1), (1, 0)]
    y = lax.axis_index("y")

    def send(v, axis, hops=swap):
        return lax.ppermute(v, axis, hops)

    def prep(which, *ins):
        wides = [wide2 if late else wide1 for _, late in which]
        held = sum(w + (LANES if late else 0) for w, (_, late) in zip(wides, which))
        return call(
            functools.partial(prep_kernel, full, first, which),
            [((blk, w), BF16) for w in wides],
            list(ins),
            in_specs=[ANY, ANY],
            scratch_shapes=[
                pltpu.VMEM((blk, held), F32),
                pltpu.SemaphoreType.DMA((4 * len(which),)),
            ],
            flops=blk * sum(wides),
            nbytes=blk * sum(wides) * 6,
        )

    (own1,) = prep(((False, False),), gate_weight, up_weight)
    far1, own2, far2 = prep(
        ((True, False), (False, True), (True, True)), after(gate_weight, own1), up_weight
    )
    hop = lambda v: send(v, "z", ahead)
    pop = lambda v: send(v, "z", back)
    c1, c2 = [own1, hop(own1)], [own2, hop(own2)]
    g1, g2 = [send(far1, "y")], [send(far2, "y")]
    n_lo, n_hi = call(
        functools.partial(norm_kernel, lo),
        [((lo, width), BF16), ((rows - lo, width), BF16)],
        [after(tokens, own2), norm_gain.reshape(1, -1)],
        flops=rows * width * 8,
        nbytes=rows * width * 4,
    )
    hi_x, hi_y = send(n_hi, "x"), send(n_hi, "y")
    d_own, d_nbr = call(
        functools.partial(down_prep_kernel, full),
        [((quarter, blk), BF16), ((quarter, blk), BF16)],
        [after(down_weight, n_hi)],
        flops=blk * ffl,
        nbytes=blk * ffl * 6,
    )
    (scale,) = call(
        functools.partial(scale_kernel, full, first),
        [((1, 2 * quarter), F32)],
        [after(v, d_own).reshape(-1, LANES) for v in (gate_scale, up_scale)],
        flops=ffl,
        nbytes=ffl * 8,
    )
    scale_oth = send(scale, "c")
    clock = scale

    def event(value):
        nonlocal clock
        clock = after(value, clock)
        return clock

    across = {}

    def twin(name, v):
        across[name] = send(v, "c")

    twin("c10", own1)
    twin("c20", own2)
    c1[1] = event(c1[1])
    c1.append(hop(c1[1]))
    twin("c11", c1[1])
    lo_x = send(after(n_lo, clock), "x")
    g1[0] = event(g1[0])
    g1.append(pop(g1[0]))
    twin("g10", g1[0])
    c2[1] = event(c2[1])
    twin("c21", c2[1])
    g2[0] = event(g2[0])
    g2.append(pop(g2[0]))
    twin("g20", g2[0])
    lo_y = send(after(n_lo, clock), "y")
    c1[2] = event(c1[2])
    c1.append(hop(c1[2]))
    twin("c12", c1[2])
    g1[1] = event(g1[1])
    g1.append(pop(g1[1]))
    twin("g11", g1[1])
    c2.append(hop(after(c2[1], clock)))
    g2[1] = event(g2[1])
    g2.append(pop(g2[1]))
    twin("g21", g2[1])
    lo_x = event(lo_x)
    lo_xy = send(lo_x, "y")
    hi_y = event(hi_y)
    hi_xy = send(hi_y, "x")
    d_far = send(after(d_nbr, clock), "y")
    c1[3] = event(c1[3])
    twin("c13", c1[3])
    g1[2] = event(g1[2])
    g1.append(pop(g1[2]))
    twin("g12", g1[2])
    c2[2] = event(c2[2])
    c2.append(hop(c2[2]))
    twin("c22", c2[2])
    g2[2] = event(g2[2])
    g2.append(pop(g2[2]))
    twin("g22", g2[2])
    d_far = event(d_far)
    even = [jnp.where(y == 0, d_own, d_far)]
    odd = [jnp.where(y == 0, d_far, d_own)]
    even.append(hop(even[0]))
    odd.append(pop(odd[0]))
    twin("e0", even[0])
    twin("o0", odd[0])
    g1[3] = event(g1[3])
    twin("g13", g1[3])
    slots = [(n_lo, n_hi), (lo_y, hi_y), (lo_x, hi_x), (lo_xy, hi_xy)]

    def gate_up(at, own, far, part, slots):
        n = wide1 if at == 1 else wide2
        wide = 2 * part + (LANES if at == 2 else 0)
        twins = [across[f"c{at}{s}"] for s in range(nz)] + [across[f"g{at}{s}"] for s in range(nz)]
        count = len(slots)
        parts = [v for slot in slots for v in slot]
        parts[0] = after(parts[0], clock)
        return call(
            functools.partial(gate_up_kernel, nz, blk, part, 0 if at == 1 else wide1, count),
            [((count * rows, wide), BF16)],
            [scale, scale_oth, *parts, *own, *far, *twins],
            in_specs=[VM, VM] + [ANY] * (2 * count + 4 * nz),
            out_specs=[pl.BlockSpec((rows, wide), lambda i: (i, 0))],
            grid=(count,),
            scratch_shapes=[
                pltpu.VMEM((count, rows, width), BF16),
                pltpu.VMEM((width, 2 * n), BF16),
                pltpu.SemaphoreType.DMA((2 * count,)),
                pltpu.SemaphoreType.DMA((4 * nz,)),
            ],
            flops=count * rows * width * n * 4,
            nbytes=count * rows * (width + wide) * 2 + width * n * 4,
        )[0]

    h1 = gate_up(1, c1, g1, first, slots)
    clock = h1
    c2[3] = event(c2[3])
    twin("c23", c2[3])
    g2[3] = event(g2[3])
    twin("g23", g2[3])
    h2 = gate_up(2, c2, g2, second, slots)
    clock = h2

    def arrive(s):
        even[s], odd[s] = event(even[s]), event(odd[s])
        if s + 1 < nz:
            even.append(hop(even[s]))
            odd.append(pop(odd[s]))
        twin(f"e{s}", even[s])
        twin(f"o{s}", odd[s])

    arrive(1)

    cuts = ((0, first), (first, full), (full, quarter))

    def down(group):
        count = len(group)
        tile = lambda n: pl.BlockSpec((2 * rows, n), lambda i: (i, 0))
        both = pl.BlockSpec((2, rows, count * blk), lambda i: (0, 0, 0))
        slot = pl.BlockSpec((1, rows, count * blk), lambda i: (i, 0, 0))
        pieces = []
        for s in group:
            pieces += [even[s], across[f"e{s}"], odd[s], across[f"o{s}"]]
        return call(
            functools.partial(down_kernel, cuts, count),
            [((2, rows, count * blk), BF16)] * 4,
            [after(h1, clock), h2, *pieces],
            in_specs=[tile(h1.shape[1]), tile(h2.shape[1])] + [ANY] * (4 * count),
            out_specs=[both, both, slot, slot],
            grid=(2,),
            scratch_shapes=[
                pltpu.VMEM((2 * quarter, 2 * count * blk), BF16),
                pltpu.SemaphoreType.DMA((4 * count * len(cuts),)),
            ],
            flops=4 * rows * quarter * 8 * blk * count,
            nbytes=4 * rows * (2 * quarter + 2 * count * blk) * 2,
        )

    def second_add(count, *ins):
        one = pl.BlockSpec((1, rows, count * blk), lambda i: (1, 0, 0))
        whole = pl.BlockSpec((rows, count * blk), lambda i: (0, 0))
        return call(
            second_add_kernel,
            [((rows, count * blk), BF16)] * 2,
            list(ins),
            grid=(1,),
            in_specs=[one] * 4,
            out_specs=[whole] * 2,
            flops=4 * rows * blk * count,
            nbytes=2 * rows * blk * 6 * count,
        )

    groups = [list(range(nz))[:2]] + [[s] for s in range(2, nz)]
    parts = []
    flying = None

    def land():
        nonlocal clock
        _, count, ax_keep, ax_got, ay_keep, ay_got = flying
        ax_got, ay_got = event(ax_got), event(ay_got)
        ax_next, ay_next = second_add(count, ax_keep, ax_got, ay_keep, ay_got)
        clock = ax_next
        parts.extend([ax_keep, ax_got, send(ax_next, "y")])
        parts.extend([ay_keep, ay_got, send(ay_next, "x")])

    for n, group in enumerate(groups):
        ax_keep, ax_send, ay_keep, ay_send = down(group)
        clock = ax_keep
        ax_got, ay_got = send(ax_send, "x"), send(ay_send, "y")
        now = (n, len(group), ax_keep, ax_got, ay_keep, ay_got)
        if flying:
            land()
        if n + 1 < len(groups):
            for s in groups[n + 1]:
                if s > 1:
                    arrive(s)
        flying = now
    land()

    def final(some, made, done):
        specs = []
        for group in some:
            third = pl.BlockSpec((1, rows, len(group) * blk), lambda i: (0, 0, 0))
            flat = pl.BlockSpec((rows, len(group) * blk), lambda i: (0, 0))
            specs += [third, third, flat] * 2
        count = 2 * sum(map(len, some))
        aliased = [] if done is None else [done]
        return call(
            functools.partial(final_kernel, nz, blk, some, bool(aliased)),
            [((rows, width), BF16)],
            [*made, down_scale.reshape(1, -1), *aliased],
            grid=(1,),
            in_specs=specs + [VM] + [ANY] * len(aliased),
            out_specs=[ANY],
            scratch_shapes=[
                pltpu.VMEM((count, rows, blk), BF16),
                pltpu.SemaphoreType.DMA((count,)),
            ],
            input_output_aliases={6 * len(some) + 1: 0} if aliased else {},
            flops=rows * count * blk * 4,
            nbytes=rows * count * blk * 8,
        )[0]

    cut = len(groups) - 1
    made = parts[: 6 * cut]
    made[0] = after(made[0], clock)
    done = final(groups[:cut], made, None)
    return final(groups[cut:], parts[6 * cut :], done)


def solution(mesh):
    reps, shards, cores = (mesh.shape[a] for a in ("rep", "fs", "tp"))

    def run(*args):
        tokens, gate = args[0], args[2]
        rows = tokens.shape[0] // (reps * shards * cores)
        ffl, blk = gate.shape[1] // cores, gate.shape[0] // shards
        paired = (
            reps == 2
            and cores == 2
            and shards % 2 == 0
            and shards > 2
            and ffl % LANES == 0
            and ffl % (4 * LANES) == 2 * LANES
            and blk % LANES == 0
            and rows % 48 == 0
        )
        if paired:
            nz = shards // 2
            grid = Mesh(mesh.devices.reshape(reps, nz, 2, cores), ("x", "z", "y", "c"))
            row, deep, wide = ("x", "z", "y", "c"), ("z", "y"), "c"
            plan = functools.partial(pair_plan, nz)

            def body(*args):
                return plan(*args)

        else:
            grid, body = mesh, general_plan
            row, deep, wide = ("rep", "fs", "tp"), "fs", "tp"
        step = jax.shard_map(
            body,
            mesh=grid,
            in_specs=(
                P(row, None),
                P(),
                P(deep, wide),
                P(deep, wide),
                P(wide),
                P(wide),
                P(wide, deep),
                P(),
            ),
            out_specs=P(row, None),
            check_vma=False,
        )
        return step(*args)

    return run
```
